32 devices in a mesh: ep: 8 (over z, core), tp: 4 (over y, x).
Axes of the slice: x: 2, y: 2, z: 4, core: 2. Of those that a mesh axis runs over, the one named last changes fastest.
Arguments:
- query_vectors: bfloat16 [4096, 4096], P('ep', 'tp'), may hold values from -6 to 6
- key_vectors: bfloat16 [4096, 2048], P('ep', 'tp'), may hold values from -6 to 6
- value_vectors: bfloat16 [4096, 2048], P('ep', 'tp'), may hold values from -64 to 64
- query_gain: float32 [128], replicated, may hold values from 0.1 to 1.9
- key_gain: float32 [128], replicated, may hold values from 0.1 to 1.9
- sink_logits: float32 [32], P('tp'), may hold values from 3 to 7
- moe_rows: bfloat16 [1280, 4096], P('ep', 'tp'), may hold values from -6 to 6
- norm_gain: float32 [4096], replicated, may hold values from 0.1 to 1.9
- expert_ids: int32 [1280, 4], P('ep'), may hold values from 0 to 7, all different within a row; in each aligned block of 160 rows (0 to 159, 160 to 319, ...) at most 120 rows name the same one
- route_weights: float32 [1280, 4], P('ep'), may hold values from 0.25 to 2.5
- expert_gate: bfloat16 [8, 4096, 2048], P('ep', None, 'tp'), may hold values from -0.09375 to 0.09375
- expert_up: bfloat16 [8, 4096, 2048], P('ep', None, 'tp'), may hold values from -0.09375 to 0.09375
- expert_down: bfloat16 [8, 2048, 4096], P('ep', None, 'tp'), may hold values from -0.125 to 0.125
- shared_gate: bfloat16 [4096, 512], P(None, 'tp'), may hold values from -0.09375 to 0.09375
- shared_up: bfloat16 [4096, 512], P(None, 'tp'), may hold values from -0.09375 to 0.09375
- shared_down: bfloat16 [512, 4096], P(None, 'tp'), may hold values from -0.25 to 0.25
Outputs:
- attended: bfloat16 [4096, 4096], P('ep', 'tp')
- moe_out: bfloat16 [1280, 4096], P('ep', 'tp')
The draws below stay inside these ranges and needn't reach their ends.
Inputs may be any that keep to these rules, and one draw needn't show every extreme that they name: `expert_ids`: each row names 4 different experts. Within the rows of one index of ep (aligned blocks of 160 rows), no expert is named by more than 120 rows, and in some block one expert is named by exactly 120.
All inputs are finite; a program needn't handle non-finite values.
Results may differ from the reference program's by a relative error of at most 0.0071.
Values may be sent and summed in bfloat16 or wider, within the bound.
A program may use at most 128 MiB of HBM per device.

```python
import math
import jax
import jax.numpy as jnp
import numpy as np
from jax import lax

HEAD_DIM = 128
HEADS = 32
KV_HEADS = 16
GROUP = 2
WINDOW = 128
GRID_W = 64
TOK_A = 512
SEQ_A = 4096
D = 4096
F = 2048
FS = 512
TOP_K = 4
TOK_B = 160
TOKENS_B = 1280
EXPERTS = 8
CAP = 120


def levels(stream_key, shape, shards, least, largest):
    def one(position, parts):
        steps = jax.random.uniform(jax.random.fold_in(jax.random.fold_in(stream_key, 6), position), (parts,), jnp.float32, least / len(shards), largest / len(shards))
        return jnp.repeat(jnp.exp(steps), shape[position] // parts).reshape((-1,) + (1,) * (len(shape) - position - 1))

    loudness = one(*shards[0])
    for cut in shards[1:]:
        loudness = loudness * one(*cut)
    return loudness


def shared_out(key, own, number, rows, number_of, top, bound, lean):
    sequence = jax.random.permutation(key, number_of)
    heavy_load, ordinary = portions_of(number_of, rows * top, bound, lean, True), portions_of(number_of, rows * top, bound, lean, False)
    places = jnp.arange(number_of)

    def named(sizes, offset_by):
        used = int((sizes > 0).sum())
        fixed = max(1, used // 4)
        shifted = fixed + (places - fixed + offset_by * (used - fixed)) % max(1, number_of - fixed)
        return jnp.zeros((number_of,), jnp.int32).at[sequence[jnp.where(places < fixed, places, shifted)]].set(jnp.asarray(sizes, jnp.int32))

    sizes = jnp.where(number % 4 == 0, named(heavy_load, number // 4), named(ordinary, number - number // 4 - 1))
    mixed = jax.random.permutation(jax.random.fold_in(own, 3), number_of)
    giver, receiver = mixed[0:number_of // 2 * 2:2], mixed[1:number_of // 2 * 2:2]
    room = jnp.minimum(sizes[giver] - 1, bound - sizes[receiver]) // 2
    room = jnp.where((giver == sequence[0]) | (receiver == sequence[0]) | (sizes[receiver] == 0), 0, jnp.maximum(room, 0))
    shifted = jax.random.randint(jax.random.fold_in(own, 4), (number_of // 2,), 0, 1 << 20) % (room + 1)
    sizes = sizes.at[giver].add(-shifted).at[receiver].add(shifted)
    items = jnp.searchsorted(jnp.cumsum(sizes), jnp.arange(rows * top), side="right").astype(jnp.int32)
    table = items.reshape(top, rows).T
    table = table[jax.random.permutation(jax.random.fold_in(own, 1), rows)]
    offset_by = jax.random.randint(jax.random.fold_in(own, 2), (rows, 1), 0, top)
    return jnp.take_along_axis(table, (jnp.arange(top)[None, :] + offset_by) % top, axis=1)


def portions_of(amount, total, most, skew, full):
    portions = [(1 << 20) // math.isqrt(standing ** skew) + 1 for standing in range(1, amount + 1)]
    largest = most if full else min(most, max(-(-total // amount), total * portions[0] // sum(portions)))
    least = 1 if total - largest >= amount - 1 else 0
    holding, rest = [largest] + [least] * (amount - 1), total - largest - least * (amount - 1)
    while rest > 0:
        free = [i for i in range(1, amount) if holding[i] < largest] or [i for i in range(1, amount) if holding[i] < most]
        pool, budget = sum([portions[i] for i in free]), rest
        for i in free:
            extra = min(most - holding[i], max(1, budget * portions[i] // pool), rest)
            holding[i] = holding[i] + extra
            rest = rest - extra
    return np.array(holding)


def gaussian(own_key, shape, width, reach, cuts=(), kind=jnp.bfloat16):
    result = width * jax.random.normal(own_key, shape, jnp.float32)
    if cuts:
        result = result * levels(own_key, shape, cuts, -0.22, 0.18)
    return jnp.clip(result, -reach, reach).astype(kind)


def setup_inputs(seed: int = 0) -> dict:
    seeds = jax.random.split(jax.random.key(seed), 17)
    query_vectors = gaussian(seeds[0], (SEQ_A, HEADS * HEAD_DIM), 1.0, 6.0, ((0, 8), (1, 4)))
    key_vectors = gaussian(seeds[1], (SEQ_A, KV_HEADS * HEAD_DIM), 1.0, 6.0, ((0, 8), (1, 4)))
    value_vectors = gaussian(seeds[2], (SEQ_A, KV_HEADS * HEAD_DIM), 12.0, 64.0, ((0, 8), (1, 4)))
    query_gain = jnp.clip(1.0 + 0.18 * jax.random.normal(seeds[3], (HEAD_DIM,), jnp.float32), 0.1, 1.9)
    key_gain = jnp.clip(1.0 + 0.18 * jax.random.normal(seeds[4], (HEAD_DIM,), jnp.float32), 0.1, 1.9)
    sink_logits = jnp.clip(3.0 + 4.0 * jax.random.uniform(seeds[5], (HEADS,), jnp.float32) ** levels(seeds[5], (HEADS,), ((0, 4),), -0.2, 0.2), 3.0, 7.0)
    moe_rows = gaussian(seeds[6], (TOKENS_B, D), 1.0, 6.0, ((0, 8), (1, 4)))
    norm_gain = jnp.clip(1.0 + 0.18 * jax.random.normal(seeds[7], (D,), jnp.float32), 0.1, 1.9)
    expert_ids_keys = jax.random.split(jax.random.fold_in(seeds[8], 1), TOKENS_B // TOK_B)
    expert_ids_turns = jax.random.permutation(jax.random.fold_in(seeds[8], 3), TOKENS_B // TOK_B)
    expert_ids = jax.vmap(lambda own, number: shared_out(jax.random.fold_in(seeds[8], 2), own, number, TOK_B, EXPERTS, TOP_K, CAP, 2))(expert_ids_keys, expert_ids_turns).reshape((TOKENS_B, TOP_K))
    route_weights = jnp.clip(jnp.exp(math.log(2.5) - 2.3025851 * jax.random.uniform(seeds[9], (TOKENS_B, TOP_K), jnp.float32) ** levels(seeds[9], (TOKENS_B, TOP_K), ((0, 8),), -0.2, 0.2)), 0.25, 2.5)
    expert_gate = gaussian(seeds[10], (EXPERTS, D, F), D ** -0.5, 0.09375, ((0, 8), (2, 4)))
    expert_up = gaussian(seeds[11], (EXPERTS, D, F), D ** -0.5, 0.09375, ((0, 8), (2, 4)))
    expert_down = gaussian(seeds[12], (EXPERTS, F, D), F ** -0.5, 0.125, ((0, 8), (2, 4)))
    shared_gate = gaussian(seeds[13], (D, FS), D ** -0.5, 0.09375, ((1, 4),))
    shared_up = gaussian(seeds[14], (D, FS), D ** -0.5, 0.09375, ((1, 4),))
    shared_down = gaussian(seeds[15], (FS, D), FS ** -0.5, 0.25, ((1, 4),))
    return dict(query_vectors=query_vectors, key_vectors=key_vectors, value_vectors=value_vectors, query_gain=query_gain, key_gain=key_gain, sink_logits=sink_logits, moe_rows=moe_rows, norm_gain=norm_gain, expert_ids=expert_ids, route_weights=route_weights, expert_gate=expert_gate, expert_up=expert_up, expert_down=expert_down, shared_gate=shared_gate, shared_up=shared_up, shared_down=shared_down)


epsilon = 1e-06
rotary_base = 10000.0

def half_turn(halves):
    leading, trailing = jnp.split(halves, 2, axis=-1)
    return jnp.concatenate([-trailing, leading], axis=-1)

def rotate_heads(vectors, head_gain, positions):
    floats = vectors.astype(jnp.float32)
    normed = floats * lax.rsqrt(lax.optimization_barrier(jnp.mean(floats * floats, axis=-1, keepdims=True)) + epsilon) * head_gain
    quarter = HEAD_DIM // 4
    freq_index = jnp.arange(quarter, dtype=jnp.int32).astype(jnp.float32)
    inverse = rotary_base ** (-4.0 * freq_index / HEAD_DIM)
    grid_row = (positions // GRID_W).astype(jnp.float32)[:, None] * inverse
    grid_col = (positions % GRID_W).astype(jnp.float32)[:, None] * inverse
    angles = jnp.concatenate([grid_row, grid_row, grid_col, grid_col], axis=-1)[:, None, :]
    row_half, col_half = jnp.split(normed, 2, axis=-1)
    turned = jnp.concatenate([half_turn(row_half), half_turn(col_half)], axis=-1)
    return (normed * jnp.cos(angles) + turned * jnp.sin(angles)).astype(jnp.bfloat16)

def activate(block_rows, gate_weight, up_weight, factor):
    gate_sum = jnp.dot(block_rows, gate_weight, preferred_element_type=jnp.float32) * factor[:, None]
    up_sum = jnp.dot(block_rows, up_weight, preferred_element_type=jnp.float32) * factor[:, None]
    return (jax.nn.silu(gate_sum) * up_sum).astype(jnp.bfloat16)

def windowed(query_vectors, key_vectors, value_vectors, query_gain, key_gain, sink_logits):
    positions = jnp.arange(SEQ_A, dtype=jnp.int32)
    queries = rotate_heads(query_vectors.reshape(SEQ_A, HEADS, HEAD_DIM), query_gain, positions)
    turned_keys = rotate_heads(key_vectors.reshape(SEQ_A, KV_HEADS, HEAD_DIM), key_gain, positions)
    values = value_vectors.reshape(SEQ_A, KV_HEADS, HEAD_DIM)
    padding = ((WINDOW, WINDOW), (0, 0), (0, 0))
    padded_keys = jnp.pad(turned_keys, padding)
    padded_values = jnp.pad(values, padding)
    blocks = SEQ_A // TOK_A
    query_blocks = queries.reshape(blocks, TOK_A, KV_HEADS, GROUP, HEAD_DIM)
    sink_scale = jnp.exp(sink_logits).reshape(KV_HEADS, GROUP)
    extent = TOK_A + 2 * WINDOW
    score_scale = HEAD_DIM ** (-0.5)

    def attend_block(packed):
        query_block, block_index = packed
        first_row = (block_index * TOK_A).astype(jnp.int32)
        near_keys = lax.dynamic_slice_in_dim(padded_keys, first_row, extent, 0)
        near_values = lax.dynamic_slice_in_dim(padded_values, first_row, extent, 0)
        query_pos = first_row + jnp.arange(TOK_A, dtype=jnp.int32)
        key_pos = first_row - WINDOW + jnp.arange(extent, dtype=jnp.int32)
        inside = (jnp.abs(query_pos[:, None] - key_pos[None, :]) <= WINDOW) & (key_pos >= 0)[None, :] & (key_pos < SEQ_A)[None, :]
        scores = jnp.einsum('qhgd,khd->hgqk', query_block.astype(jnp.float32), near_keys.astype(jnp.float32)) * score_scale
        raised = jnp.where(inside, jnp.exp(scores), 0.0)
        denominator = sink_scale[:, :, None] + lax.optimization_barrier(jnp.sum(raised, axis=-1))
        weights = (raised / denominator[..., None]).astype(jnp.bfloat16)
        mixed = jnp.einsum('hgqk,khd->qhgd', weights.astype(jnp.float32), near_values.astype(jnp.float32))
        return mixed.astype(jnp.bfloat16).reshape(TOK_A, HEADS * HEAD_DIM)
    outputs = lax.map(attend_block, (query_blocks, jnp.arange(blocks, dtype=jnp.int32)))
    return outputs.reshape(SEQ_A, HEADS * HEAD_DIM)

def moe_layer(moe_rows, norm_gain, expert_ids, route_weights, expert_gate, expert_up, expert_down, shared_gate, shared_up, shared_down):
    floats = moe_rows.astype(jnp.float32)
    inverse_rms = lax.rsqrt(lax.optimization_barrier(jnp.mean(floats * floats, axis=-1)) + epsilon)
    scaled = (floats * norm_gain).astype(jnp.bfloat16)
    shared_hidden = activate(scaled, shared_gate, shared_up, inverse_rms)
    shared_result = jnp.dot(shared_hidden, shared_down, preferred_element_type=jnp.float32)
    blocks = TOKENS_B // TOK_B
    flat_ids = expert_ids.reshape(blocks, TOK_B * TOP_K).astype(jnp.int32)
    onehot = (flat_ids[:, :, None] == jnp.arange(EXPERTS, dtype=jnp.int32)[None, None, :]).astype(jnp.int32)
    slot_index = lax.optimization_barrier(jnp.sum((jnp.cumsum(onehot, axis=1) - onehot) * onehot, axis=-1)).astype(jnp.int32)
    owner_row = jnp.arange(TOK_B * TOP_K, dtype=jnp.int32) // TOP_K
    scaled_blocks = scaled.reshape(blocks, TOK_B, D)
    rms_blocks = inverse_rms.reshape(blocks, TOK_B)
    capacity_index = jnp.arange(CAP, dtype=jnp.int32)

    def one_expert(packed):
        expert, gate_weight, up_weight, down_weight = packed
        matches = (flat_ids == expert)[:, :, None] & (slot_index[:, :, None] == capacity_index[None, None, :])
        present = jnp.any(matches, axis=1)
        source_row = lax.optimization_barrier(jnp.sum(jnp.where(matches, owner_row[None, :, None], 0), axis=1)).astype(jnp.int32)
        picked = jnp.take_along_axis(scaled_blocks, source_row[:, :, None], axis=1)
        picked = jnp.where(present[:, :, None], picked, jnp.zeros((), jnp.bfloat16))
        factor = jnp.where(present, jnp.take_along_axis(rms_blocks, source_row, axis=1), 0.0)
        hidden = activate(picked.reshape(blocks * CAP, D), gate_weight, up_weight, factor.reshape(blocks * CAP))
        return jnp.dot(hidden, down_weight, preferred_element_type=jnp.float32).astype(jnp.bfloat16).reshape(blocks, CAP, D)
    results = lax.map(one_expert, (jnp.arange(EXPERTS, dtype=jnp.int32), expert_gate, expert_up, expert_down))
    block_ids = expert_ids.reshape(blocks, TOK_B, TOP_K).astype(jnp.int32)
    block_slots = slot_index.reshape(blocks, TOK_B, TOP_K)
    source_block = jnp.arange(blocks, dtype=jnp.int32)[:, None, None]
    gathered = results[block_ids, source_block, block_slots]
    routed = lax.optimization_barrier(jnp.sum(route_weights.reshape(blocks, TOK_B, TOP_K, 1) * gathered.astype(jnp.float32), axis=2))
    return (shared_result + routed.reshape(TOKENS_B, D)).astype(jnp.bfloat16)

def reference(query_vectors, key_vectors, value_vectors, query_gain, key_gain, sink_logits, moe_rows, norm_gain, expert_ids, route_weights, expert_gate, expert_up, expert_down, shared_gate, shared_up, shared_down):
    attended = windowed(query_vectors, key_vectors, value_vectors, query_gain, key_gain, sink_logits)
    moe_out = moe_layer(moe_rows, norm_gain, expert_ids, route_weights, expert_gate, expert_up, expert_down, shared_gate, shared_up, shared_down)
    return (attended, moe_out)
```

```python
import functools

import jax
import jax.numpy as jnp
from jax import lax
from jax.experimental import pallas as pl
from jax.experimental.pallas import tpu as pltpu
from jax.sharding import PartitionSpec as P

HEAD_DIM = 128
WINDOW = 128
GRID_W = 64
D = 4096
TOP_K = 4


epsilon = 1e-06
rotary_base = 10000.0


def padded_2(block, sides, width):
    for axis, dim in sides:
        count = lax.axis_size(axis)
        forward = [(i, i + 1) for i in range(count - 1)]
        backward = [(target, source) for source, target in forward]
        low = lax.ppermute(
            lax.slice_in_dim(block, block.shape[dim] - width, None, axis=dim), axis, forward
        )
        high = lax.ppermute(lax.slice_in_dim(block, 0, width, axis=dim), axis, backward)
        block = jnp.concatenate([low, block, high], axis=dim)
    return block


def half_turn(halves):
    leading, trailing = jnp.split(halves, 2, axis=-1)
    return jnp.concatenate([-trailing, leading], axis=-1)


def rotate_heads(vectors, head_gain, positions):
    floats = vectors.astype(jnp.float32)
    normed = (
        floats * lax.rsqrt(jnp.mean(floats * floats, axis=-1, keepdims=True) + epsilon) * head_gain
    )
    quarter = HEAD_DIM // 4
    freq_index = jnp.arange(quarter, dtype=jnp.int32).astype(jnp.float32)
    inverse = rotary_base ** (-4.0 * freq_index / HEAD_DIM)
    grid_row = (positions // GRID_W).astype(jnp.float32)[:, None] * inverse
    grid_col = (positions % GRID_W).astype(jnp.float32)[:, None] * inverse
    angles = jnp.concatenate([grid_row, grid_row, grid_col, grid_col], axis=-1)[:, None, :]
    row_half, col_half = jnp.split(normed, 2, axis=-1)
    turned = jnp.concatenate([half_turn(row_half), half_turn(col_half)], axis=-1)
    return (normed * jnp.cos(angles) + turned * jnp.sin(angles)).astype(jnp.bfloat16)


def attend_window(query_vectors, key_vectors, value_vectors, query_gain, key_gain, sink_logits):
    length = query_vectors.shape[0]
    heads_here = sink_logits.shape[0]
    kv_here = key_vectors.shape[1] // HEAD_DIM
    grouping = heads_here // kv_here
    shard_start = lax.axis_index("ep") * length
    positions = shard_start + jnp.arange(length, dtype=jnp.int32)
    queries = rotate_heads(
        query_vectors.reshape(length, heads_here, HEAD_DIM), query_gain, positions
    )
    turned_keys = rotate_heads(key_vectors.reshape(length, kv_here, HEAD_DIM), key_gain, positions)
    turned_keys = turned_keys.reshape(length, kv_here * HEAD_DIM)
    padded = padded_2(jnp.stack([turned_keys, value_vectors]), (("ep", 1),), WINDOW)
    extent = length + 2 * WINDOW
    near_keys = padded[0].reshape(extent, kv_here, HEAD_DIM)
    near_values = padded[1].reshape(extent, kv_here, HEAD_DIM)
    key_pos = shard_start - WINDOW + jnp.arange(extent, dtype=jnp.int32)
    inside = (
        (jnp.abs(positions[:, None] - key_pos[None, :]) <= WINDOW)
        & (key_pos >= 0)[None, :]
        & (key_pos < lax.axis_size("ep") * length)[None, :]
    )
    scores = jnp.einsum(
        "qhgd,khd->hgqk",
        queries.reshape(length, kv_here, grouping, HEAD_DIM),
        near_keys,
        preferred_element_type=jnp.float32,
    ) * HEAD_DIM ** (-0.5)
    raised = jnp.where(inside, jnp.exp(scores), 0.0)
    denominator = jnp.exp(sink_logits).reshape(kv_here, grouping)[:, :, None] + jnp.sum(
        raised, axis=-1
    )
    weights = (raised / denominator[..., None]).astype(jnp.bfloat16)
    mixed = jnp.einsum("hgqk,khd->qhgd", weights, near_values, preferred_element_type=jnp.float32)
    return mixed.astype(jnp.bfloat16).reshape(length, heads_here * HEAD_DIM)


def project(block_rows, gain_piece, gate_rows, up_rows):
    floats = block_rows.astype(jnp.float32)
    weighted = (floats * gain_piece).astype(jnp.bfloat16)
    gate_sum = jnp.dot(weighted, gate_rows, preferred_element_type=jnp.float32)
    up_sum = jnp.dot(weighted, up_rows, preferred_element_type=jnp.float32)
    return (gate_sum, up_sum, jnp.sum(floats * floats, axis=1))


def activate(gate_sum, up_sum, squares):
    factor = lax.rsqrt(squares / D + epsilon)[:, None]
    return (jax.nn.silu(gate_sum * factor) * (up_sum * factor)).astype(jnp.bfloat16)


def shards(
    query_vectors,
    key_vectors,
    value_vectors,
    query_gain,
    key_gain,
    sink_logits,
    moe_rows,
    norm_gain,
    expert_ids,
    route_weights,
    expert_gate,
    expert_up,
    expert_down,
    shared_gate,
    shared_up,
    shared_down,
):
    attended = attend_window(
        query_vectors, key_vectors, value_vectors, query_gain, key_gain, sink_logits
    )
    ep_size = lax.axis_size("ep")
    tokens_here, width_here = moe_rows.shape
    capacity = max(2, 3 * tokens_here * TOP_K // (2 * ep_size))
    slots_all = ep_size * capacity
    flat_ids = expert_ids.reshape(-1)
    onehot = (flat_ids[:, None] == jnp.arange(ep_size, dtype=jnp.int32)[None, :]).astype(jnp.int32)
    slot_index = jnp.sum((jnp.cumsum(onehot, axis=0) - onehot) * onehot, axis=1)
    target = flat_ids * capacity + slot_index
    matches = target[None, :] == jnp.arange(slots_all, dtype=jnp.int32)[:, None]
    present = jnp.any(matches, axis=1)
    owner_row = jnp.arange(tokens_here * TOP_K, dtype=jnp.int32) // TOP_K
    source_row = jnp.sum(jnp.where(matches, owner_row[None, :], 0), axis=1)
    local_gate = expert_gate[0]
    local_up = expert_up[0]
    local_down = expert_down[0]
    units_here = local_gate.shape[1]
    shared_units = shared_gate.shape[1]
    outgoing = jnp.where(
        present[:, None], jnp.take(moe_rows, source_row, axis=0), jnp.zeros((), jnp.bfloat16)
    )
    arrived = lax.all_to_all(
        outgoing.reshape(ep_size, capacity, width_here),
        "ep",
        split_axis=0,
        concat_axis=0,
        tiled=True,
    )
    arrived = arrived.reshape(slots_all, width_here)
    routed = project(
        lax.all_gather(arrived, "tp", axis=1, tiled=True), norm_gain, local_gate, local_up
    )
    shared = project(
        lax.all_gather(moe_rows, "tp", axis=1, tiled=True), norm_gain, shared_gate, shared_up
    )
    gate_sum, up_sum, squares, shared_gsum, shared_usum, own_squares = tuple(
        (new_term for new_term in routed + shared)
    )
    hidden = activate(gate_sum, up_sum, squares)
    shared_hidden = activate(shared_gsum, shared_usum, own_squares)
    packing = units_here // shared_units
    stacked = jnp.concatenate(
        [hidden, shared_hidden.reshape(tokens_here // packing, units_here)], axis=0
    )
    columns = local_down.shape[1]
    portion = lax.all_gather(stacked, "tp", axis=1, tiled=True)
    shards_in = portion.shape[1] // units_here
    routed = jnp.dot(portion[:slots_all], local_down, preferred_element_type=jnp.float32)
    shared_piece = portion[slots_all:].reshape(
        tokens_here // packing, shards_in, packing, shared_units
    )
    shared_piece = shared_piece.transpose(0, 2, 1, 3).reshape(tokens_here, shards_in * shared_units)
    shared = jnp.dot(shared_piece, shared_down, preferred_element_type=jnp.float32)
    returned = lax.all_to_all(
        routed.astype(jnp.bfloat16).reshape(ep_size, capacity, columns),
        "ep",
        split_axis=0,
        concat_axis=0,
        tiled=True,
    )
    returned = returned.reshape(slots_all, columns)
    picked = jnp.take(returned, target, axis=0).reshape(tokens_here, TOP_K, columns)
    combined = shared + jnp.sum(route_weights[:, :, None] * picked.astype(jnp.float32), axis=1)
    return (attended, combined.astype(jnp.bfloat16))


F32 = jnp.float32
BF16 = jnp.bfloat16
MESH = pl.DeviceIdType.MESH
LANES = 128


def moe_kernel(
    sizes,
    q_hbm,
    k_hbm,
    v_hbm,
    cos_ref,
    sin_ref,
    qgain_ref,
    kgain_ref,
    sink_ref,
    x_hbm,
    gain_ref,
    wt_hbm,
    gate_hbm,
    up_hbm,
    down_hbm,
    sgate_hbm,
    sup_hbm,
    sdown_hbm,
    att_ref,
    out_ref,
    xbuf,
    gate,
    up,
    down,
    sgate,
    sup,
    sdown,
    qbuf,
    kbuf,
    vbuf,
    wbuf,
    scaled,
    factor,
    hid,
    hbuf,
    shbuf,
    pbuf,
    prx,
    qtx,
    qrx,
    local_sem,
    zs,
    zr,
    xs,
    xr,
    ys,
    yr,
    dxs,
    dxr,
    dys,
    dyr,
    ps,
    pr,
    hxs,
    hxr,
    hys,
    hyr,
    gxs,
    gxr,
    gys,
    gyr,
    ss,
    sr,
    ws,
    wr,
    ks,
    kr,
    pps,
    ppr,
    qqs,
    qqr,
):
    ep, tp, nz, tok, width, cap, tok_a, kv_heads, group, units, columns, sunits = sizes
    e = lax.axis_index("ep")
    t = lax.axis_index("tp")
    z, c = e // 2, e % 2
    other = 1 - c
    partner = z * 2 + other
    tx, ty = t % 2, t // 2
    xn = ty * 2 + (1 - tx)
    yn = (1 - ty) * 2 + tx
    dn = (1 - ty) * 2 + (1 - tx)
    half = tok // 2
    slots = 2 * cap
    hcut = (slots // 2 + 15) // 16 * 16
    row_c = pl.multiple_of(c * tok, 16)
    row_o = pl.multiple_of(other * tok, 16)

    def rc(src, dst, s_sem, r_sem, dev):
        return pltpu.make_async_remote_copy(
            src_ref=src,
            dst_ref=dst,
            send_sem=s_sem,
            recv_sem=r_sem,
            device_id=dev,
            device_id_type=MESH,
        )

    unit0 = xbuf.at[z, t, pl.ds(row_c, tok), :]
    loads = [
        (x_hbm, unit0),
        (wt_hbm, wbuf.at[e]),
        (k_hbm, kbuf.at[pl.ds(WINDOW, tok_a), :]),
        (v_hbm, vbuf.at[pl.ds(WINDOW, tok_a), :]),
        (q_hbm, qbuf),
        (gate_hbm.at[0], gate),
        (up_hbm.at[0], up),
        (sgate_hbm, sgate),
        (sup_hbm, sup),
        (down_hbm.at[0], down),
        (sdown_hbm, sdown),
    ]
    copies = [
        pltpu.make_async_copy(a, b, local_sem.at[i]) for i, (a, b) in enumerate(loads)
    ]
    for cp in copies:
        cp.start()

    barrier = pltpu.get_barrier_semaphore()
    for d in range(1, ep):
        pl.semaphore_signal(barrier, inc=1, device_id=((e + d) % ep, t), device_id_type=MESH)
    for d in range(1, tp):
        pl.semaphore_signal(barrier, inc=1, device_id=(e, (t + d) % tp), device_id_type=MESH)
    pl.semaphore_wait(barrier, ep + tp - 2)

    def unit(zi, ti, row, first=0, count=tok):
        return xbuf.at[zi, ti, pl.ds(row + first, count), :]

    def z_copy(d):
        zi = (z + d) % nz
        return rc(unit0, unit0, zs.at[d], zr.at[z], (zi * 2 + c, t))

    def z_landed(zi):
        u = unit(zi, t, row_c)
        return rc(u, u, zs.at[0], zr.at[zi], (e, xn))

    def x_copy(zi):
        u = unit(zi, t, row_c)
        return rc(u, u, xs.at[zi], xr.at[zi], (e, xn))

    def y_copy(zi):
        u = unit(zi, t, row_c)
        return rc(u, u, ys.at[zi], yr.at[zi], (e, yn))

    def x_landed(zi):
        u = unit(zi, xn, row_c)
        return rc(u, u, xs.at[zi], xr.at[zi], (e, xn))

    def y_landed(zi):
        u = unit(zi, yn, row_c)
        return rc(u, u, ys.at[zi], yr.at[zi], (e, yn))

    def dy_copy(zi):
        u = unit(zi, xn, row_c, 0, half)
        return rc(u, u, dys.at[zi], dyr.at[zi], (e, yn))

    def dx_copy(zi):
        u = unit(zi, yn, row_c, half, half)
        return rc(u, u, dxs.at[zi], dxr.at[zi], (e, xn))

    def dy_landed(zi):
        u = unit(zi, dn, row_c, 0, half)
        return rc(u, u, dys.at[zi], dyr.at[zi], (e, yn))

    def dx_landed(zi):
        u = unit(zi, dn, row_c, half, half)
        return rc(u, u, dxs.at[zi], dxr.at[zi], (e, xn))

    def p_copy(zi, ti):
        u = unit(zi, ti, row_c)
        return rc(u, u, ps.at[zi, ti], pr.at[zi, ti], (partner, t))

    def p_landed(zi, ti):
        u = unit(zi, ti, row_o)
        return rc(u, u, ps.at[zi, ti], pr.at[zi, ti], (partner, t))

    def hx_copy(zi):
        u = hbuf.at[zi, t]
        return rc(u, u, hxs.at[zi], hxr.at[zi], (e, xn))

    def hy_copy(zi):
        u = hbuf.at[zi, t]
        return rc(u, u, hys.at[zi], hyr.at[zi], (e, yn))

    def hx_landed(zi):
        u = hbuf.at[zi, xn]
        return rc(u, u, hxs.at[zi], hxr.at[zi], (e, xn))

    def hy_landed(zi):
        u = hbuf.at[zi, yn]
        return rc(u, u, hys.at[zi], hyr.at[zi], (e, yn))

    def gy_copy(zi):
        u = hbuf.at[zi, xn, pl.ds(0, hcut), :]
        return rc(u, u, gys.at[zi], gyr.at[zi], (e, yn))

    def gx_copy(zi):
        u = hbuf.at[zi, yn, pl.ds(hcut, slots - hcut), :]
        return rc(u, u, gxs.at[zi], gxr.at[zi], (e, xn))

    def gy_landed(zi):
        u = hbuf.at[zi, dn, pl.ds(0, hcut), :]
        return rc(u, u, gys.at[zi], gyr.at[zi], (e, yn))

    def gx_landed(zi):
        u = hbuf.at[zi, dn, pl.ds(hcut, slots - hcut), :]
        return rc(u, u, gxs.at[zi], gxr.at[zi], (e, xn))

    def s_copy(d):
        u = shbuf.at[t]
        return rc(u, u, ss.at[d], sr.at[t], (e, (t + d) % tp))

    def s_landed(ti):
        u = shbuf.at[ti]
        return rc(u, u, ss.at[0], sr.at[ti], (e, xn))

    def w_copy(d):
        u = wbuf.at[e]
        return rc(u, u, ws.at[d], wr.at[e], ((e + d) % ep, t))

    def w_landed(ei):
        u = wbuf.at[ei]
        return rc(u, u, ws.at[0], wr.at[ei], (partner, t))

    after, before = (e + 1) % ep, (e + ep - 1) % ep
    tail = pl.ds(tok_a, WINDOW)
    first = pl.ds(WINDOW, WINDOW)
    low = pl.ds(0, WINDOW)
    high = pl.ds(WINDOW + tok_a, WINDOW)
    halos = [
        rc(kbuf.at[tail, :], kbuf.at[low, :], ks.at[0], kr.at[0], (after, t)),
        rc(kbuf.at[first, :], kbuf.at[high, :], ks.at[1], kr.at[1], (before, t)),
        rc(vbuf.at[tail, :], vbuf.at[low, :], ks.at[2], kr.at[2], (after, t)),
        rc(vbuf.at[first, :], vbuf.at[high, :], ks.at[3], kr.at[3], (before, t)),
    ]

    def pp_copy(zi):
        return rc(pbuf.at[zi, other], prx.at[zi], pps.at[zi], ppr.at[zi], (partner, t))

    def qq_copy(zi):
        return rc(qtx.at[zi], qrx.at[z], qqs.at[zi], qqr.at[z], (zi * 2 + c, t))

    def qq_landed(zi):
        return rc(qrx.at[zi], qrx.at[zi], qqs.at[zi], qqr.at[zi], (partner, t))

    copies[0].wait()
    x_copy(z).start()
    y_copy(z).start()
    for d in range(1, nz):
        z_copy(d).start()
    p_copy(z, t).start()
    copies[1].wait()
    for d in range(1, ep):
        w_copy(d).start()
    copies[2].wait()
    copies[3].wait()
    for h in halos:
        h.start()
    copies[4].wait()

    lane = lax.broadcasted_iota(jnp.int32, (WINDOW, LANES), 1)
    leading = (lane % (HEAD_DIM // 2)) < HEAD_DIM // 4

    def turn(block, head_gain, table_rows):
        v = block.astype(F32)
        v = v * lax.rsqrt(jnp.mean(v * v, axis=-1, keepdims=True) + epsilon) * head_gain
        swapped = jnp.where(
            leading,
            pltpu.roll(v, HEAD_DIM - HEAD_DIM // 4, 1),
            pltpu.roll(v, HEAD_DIM // 4, 1),
        )
        return (v * cos_ref[table_rows, :] + swapped * sin_ref[table_rows, :]).astype(BF16)

    heads = kv_heads * group

    def turn_q(i, carry):
        rows = pl.ds(pl.multiple_of(i * WINDOW, WINDOW), WINDOW)
        table = pl.ds(pl.multiple_of((i + 1) * WINDOW, WINDOW), WINDOW)
        for h in range(heads):
            cols = slice(h * HEAD_DIM, (h + 1) * HEAD_DIM)
            qbuf[rows, cols] = turn(qbuf[rows, cols], qgain_ref[...], table)
        return carry

    nq = tok_a // WINDOW
    lax.fori_loop(0, nq, turn_q, 0)

    def forward_z(zi):
        z_landed(zi).wait_recv()
        x_copy(zi).start()
        y_copy(zi).start()
        p_copy(zi, t).start()

    forward_z((z + 1) % nz)

    for h in halos:
        h.wait()

    def turn_k(i, carry):
        rows = pl.ds(pl.multiple_of(i * WINDOW, WINDOW), WINDOW)
        for h in range(kv_heads):
            cols = slice(h * HEAD_DIM, (h + 1) * HEAD_DIM)
            kbuf[rows, cols] = turn(kbuf[rows, cols], kgain_ref[...], rows)
        return carry

    lax.fori_loop(0, nq + 2, turn_k, 0)
    for d in range(1, ep):
        w_landed((e + d) % ep).wait_recv()
    for cp in copies[5:]:
        cp.wait()

    span = 3 * WINDOW

    def attend(i, carry):
        qb, kh = i // kv_heads, i % kv_heads
        rows = pl.ds(pl.multiple_of(qb * WINDOW, WINDOW), WINDOW)
        keys = pl.ds(pl.multiple_of(qb * WINDOW, WINDOW), span)
        kcols = pl.ds(pl.multiple_of(kh * HEAD_DIM, HEAD_DIM), HEAD_DIM)
        near = lax.broadcasted_iota(jnp.int32, (WINDOW, span), 1)
        mine = lax.broadcasted_iota(jnp.int32, (WINDOW, span), 0)
        pos = e * tok_a + (qb - 1) * WINDOW + near
        inside = (
            (near - mine >= 0) & (near - mine <= 2 * WINDOW) & (pos >= 0) & (pos < ep * tok_a)
        )
        kk = kbuf[keys, kcols]
        vv = vbuf[keys, kcols]
        for g in range(group):
            qcols = pl.ds(
                pl.multiple_of((kh * group + g) * HEAD_DIM, HEAD_DIM), HEAD_DIM
            )
            scores = lax.dot_general(
                qbuf[rows, qcols], kk, (((1,), (1,)), ((), ())), preferred_element_type=F32
            )
            raised = jnp.where(inside, jnp.exp(scores * HEAD_DIM ** (-0.5)), 0.0)
            sink = jnp.exp(sink_ref[kh * group + g])
            total = jnp.sum(raised, axis=-1, keepdims=True) + sink[0:1, 0:1]
            weights = (raised * (1.0 / total)).astype(BF16)
            att_ref[rows, qcols] = jnp.dot(weights, vv, preferred_element_type=F32).astype(BF16)
        return carry

    upper = (
        lax.broadcasted_iota(jnp.int32, (tok, tok), 0)
        < lax.broadcasted_iota(jnp.int32, (tok, tok), 1)
    ).astype(F32)

    def picks(block):
        weight = wbuf[block, pl.ds(e, 1), :][:, :tok]
        named = jnp.where(weight > 0.0, 1.0, 0.0)
        rank = jnp.dot(
            jnp.broadcast_to(named, (16, tok)).astype(BF16),
            upper.astype(BF16),
            preferred_element_type=F32,
        )[0:1, :]
        slot = lax.broadcasted_iota(jnp.int32, (cap, tok), 0).astype(F32)
        hot = jnp.where((slot == rank) & (named > 0.0), 1.0, 0.0)
        return hot, jnp.sum(hot * weight, axis=1, keepdims=True)

    chunk = 32

    def silu_pair(g, u, f):
        g = g * f
        return g / (1.0 + jnp.exp(-g)) * (u * f)

    tile = min(256, units)

    def project_pair(zi):
        def scale(i, carry):
            rows = pl.ds(pl.multiple_of(i * chunk, chunk), chunk)
            squares = jnp.zeros((chunk, 1), F32)
            for ti in range(tp):
                v = xbuf[zi, ti, rows, :].astype(F32)
                squares += jnp.sum(v * v, axis=1, keepdims=True)
                cols = slice(ti * width, (ti + 1) * width)
                scaled[rows, cols] = (v * gain_ref[:, cols]).astype(BF16)
            f = lax.rsqrt(squares / (tp * width) + epsilon)
            factor[rows, :] = jnp.broadcast_to(f, (chunk, LANES))
            return carry

        lax.fori_loop(0, 2 * tok // chunk, scale, 0)

        def columns_of(n, carry):
            cols = pl.ds(pl.multiple_of(n * tile, tile), tile)
            g = jnp.dot(scaled[...], gate[:, cols], preferred_element_type=F32)
            u = jnp.dot(scaled[...], up[:, cols], preferred_element_type=F32)
            hid[:, cols] = silu_pair(g, u, factor[:, 0:1]).astype(BF16)
            return carry

        lax.fori_loop(0, units // tile, columns_of, 0)
        parts = []
        for ci in range(2):
            hot, _ = picks(zi * 2 + ci)
            parts.append(
                jnp.dot(
                    hot.astype(BF16),
                    hid[ci * tok : (ci + 1) * tok, :],
                    preferred_element_type=F32,
                )
            )
        hbuf[zi, t] = jnp.concatenate(parts, axis=0).astype(BF16)

    def shared_up():
        rows = pl.ds(row_c, tok)
        g = jnp.dot(scaled[rows, :], sgate[...], preferred_element_type=F32)
        u = jnp.dot(scaled[rows, :], sup[...], preferred_element_type=F32)
        shbuf[t] = silu_pair(g, u, factor[rows, 0:1]).astype(BF16)

    ctile = min(256, columns)

    def down_pair(zi):
        picked = [picks(zi * 2 + ci) for ci in range(2)]
        slot_weight = jnp.concatenate([p[1] for p in picked], axis=0)

        def columns_of(n, carry):
            cols = pl.ds(pl.multiple_of(n * ctile, ctile), ctile)
            acc = jnp.zeros((slots, ctile), F32)
            for ti in range(tp):
                acc += jnp.dot(
                    hbuf[zi, ti],
                    down[ti * units : (ti + 1) * units, cols],
                    preferred_element_type=F32,
                )
            weighted = acc.astype(BF16).astype(F32) * slot_weight
            for ci in range(2):
                spread = lax.dot_general(
                    picked[ci][0].astype(BF16),
                    weighted[ci * cap : (ci + 1) * cap, :].astype(BF16),
                    (((0,), (0,)), ((), ())),
                    preferred_element_type=F32,
                )
                pbuf[zi, ci, :, cols] = spread.astype(BF16)
            return carry

        lax.fori_loop(0, columns // ctile, columns_of, 0)

    per_step = nq * kv_heads // nz

    def step(s, carry):
        @pl.when(s < nz)
        def _():
            lax.fori_loop(s * per_step, (s + 1) * per_step, attend, 0)
            zi = (z + s) % nz
            x_landed(zi).wait_recv()
            dy_copy(zi).start()
            p_copy(zi, xn).start()
            y_landed(zi).wait_recv()
            dx_copy(zi).start()
            p_copy(zi, yn).start()

            @pl.when(s + 2 < nz)
            def _():
                forward_z((z + s + 2) % nz)

            dy_landed(zi).wait_recv()
            dx_landed(zi).wait_recv()
            p_copy(zi, dn).start()
            for ti in range(tp):
                p_landed(zi, ti).wait_recv()
            project_pair(zi)
            hx_copy(zi).start()
            hy_copy(zi).start()

            @pl.when(s == 0)
            def _():
                shared_up()
                for d in range(1, tp):
                    s_copy(d).start()

        @pl.when((s >= 1) & (s < nz + 1))
        def _():
            zi = (z + s - 1) % nz
            hx_landed(zi).wait_recv()
            gy_copy(zi).start()
            hy_landed(zi).wait_recv()
            gx_copy(zi).start()

        @pl.when((s >= 2) & (s < nz + 2))
        def _():
            zi = (z + s - 2) % nz
            gy_landed(zi).wait_recv()
            gx_landed(zi).wait_recv()
            down_pair(zi)
            pp_copy(zi).start()
            pp_copy(zi).wait_recv()
            qtx[zi] = (pbuf[zi, c].astype(F32) + prx[zi].astype(F32)).astype(BF16)

            @pl.when(s > 2)
            def _():
                qq_copy(zi).start()

        return carry

    lax.fori_loop(0, nz + 2, step, 0)

    for d in range(1, tp):
        s_landed((t + d) % tp).wait_recv()
    for d in range(1, nz):
        qq_landed((z + d) % nz).wait_recv()
    for n in range(columns // ctile):
        cols = slice(n * ctile, (n + 1) * ctile)
        acc = qtx[z, :, cols].astype(F32)
        for d in range(1, nz):
            acc += qrx[(z + d) % nz, :, cols].astype(F32)
        for ti in range(tp):
            acc += jnp.dot(
                shbuf[ti],
                sdown[ti * sunits : (ti + 1) * sunits, cols],
                preferred_element_type=F32,
            )
        out_ref[:, cols] = acc.astype(BF16)

    for d in range(1, nz):
        z_copy(d).wait_send()
        qq_copy((z + d) % nz).wait_send()
    for d in range(1, tp):
        s_copy(d).wait_send()
    for d in range(1, ep):
        w_copy(d).wait_send()

    def drain(zi, carry):
        for kind in (x_copy, y_copy, dx_copy, dy_copy, hx_copy, hy_copy, gx_copy, gy_copy, pp_copy):
            kind(zi).wait_send()
        for ti in range(tp):
            p_copy(zi, ti).wait_send()
        return carry

    lax.fori_loop(0, nz, drain, 0)


def fast_shards(
    query_vectors,
    key_vectors,
    value_vectors,
    query_gain,
    key_gain,
    sink_logits,
    moe_rows,
    norm_gain,
    expert_ids,
    route_weights,
    expert_gate,
    expert_up,
    expert_down,
    shared_gate,
    shared_up,
    shared_down,
):
    ep, tp = lax.axis_size("ep"), lax.axis_size("tp")
    nz = ep // 2
    tok, width = moe_rows.shape
    cap = max(2, 3 * tok * TOP_K // (2 * ep))
    tok_a = query_vectors.shape[0]
    heads = sink_logits.shape[0]
    kv_heads = key_vectors.shape[1] // HEAD_DIM
    group = heads // kv_heads
    units = expert_gate.shape[2]
    columns = expert_down.shape[2]
    sunits = shared_gate.shape[1]
    sizes = (ep, tp, nz, tok, width, cap, tok_a, kv_heads, group, units, columns, sunits)
    full = tp * width

    extent = tok_a + 2 * WINDOW
    positions = lax.axis_index("ep") * tok_a - WINDOW + jnp.arange(extent, dtype=jnp.int32)
    quarter = HEAD_DIM // 4
    inverse = rotary_base ** (-4.0 * jnp.arange(quarter, dtype=jnp.int32).astype(F32) / HEAD_DIM)
    grid_row = (positions // GRID_W).astype(F32)[:, None] * inverse
    grid_col = (positions % GRID_W).astype(F32)[:, None] * inverse
    cr, cc, sr, sc = jnp.cos(grid_row), jnp.cos(grid_col), jnp.sin(grid_row), jnp.sin(grid_col)
    cos = jnp.concatenate([cr, cr, cc, cc], axis=-1)
    sin = jnp.concatenate([-sr, sr, -sc, sc], axis=-1)

    experts = jnp.arange(ep, dtype=jnp.int32)
    table = jnp.sum(
        jnp.where(expert_ids.T[None, :, :] == experts[:, None, None], route_weights.T[None], 0.0),
        axis=1,
    )
    padded_tok = (tok + LANES - 1) // LANES * LANES
    table = jnp.pad(table, ((0, 0), (0, padded_tok - tok)))
    sinks = jnp.broadcast_to(sink_logits[:, None, None], (heads, 8, LANES))

    vm = pl.BlockSpec(memory_space=pltpu.VMEM)
    hb = pl.BlockSpec(memory_space=pl.ANY)
    dma = pltpu.SemaphoreType.DMA
    slots = 2 * cap
    zz = [dma((nz,))] * 2
    return pl.pallas_call(
        functools.partial(moe_kernel, sizes),
        out_shape=(
            jax.ShapeDtypeStruct((tok_a, heads * HEAD_DIM), BF16),
            jax.ShapeDtypeStruct((tok, columns), BF16),
        ),
        in_specs=[hb, hb, hb, vm, vm, vm, vm, vm, hb, vm, hb, hb, hb, hb, hb, hb, hb],
        out_specs=(vm, vm),
        scratch_shapes=[
            pltpu.VMEM((nz, tp, 2 * tok, width), BF16),
            pltpu.VMEM((full, units), BF16),
            pltpu.VMEM((full, units), BF16),
            pltpu.VMEM((tp * units, columns), BF16),
            pltpu.VMEM((full, sunits), BF16),
            pltpu.VMEM((full, sunits), BF16),
            pltpu.VMEM((tp * sunits, columns), BF16),
            pltpu.VMEM((tok_a, heads * HEAD_DIM), BF16),
            pltpu.VMEM((extent, kv_heads * HEAD_DIM), BF16),
            pltpu.VMEM((extent, kv_heads * HEAD_DIM), BF16),
            pltpu.VMEM((ep, ep, padded_tok), F32),
            pltpu.VMEM((2 * tok, full), BF16),
            pltpu.VMEM((2 * tok, LANES), F32),
            pltpu.VMEM((2 * tok, units), BF16),
            pltpu.VMEM((nz, tp, slots, units), BF16),
            pltpu.VMEM((tp, tok, sunits), BF16),
            pltpu.VMEM((nz, 2, tok, columns), BF16),
            pltpu.VMEM((nz, tok, columns), BF16),
            pltpu.VMEM((nz, tok, columns), BF16),
            pltpu.VMEM((nz, tok, columns), BF16),
            dma((11,)),
        ]
        + zz * 5
        + [dma((nz, tp))] * 2
        + zz * 4
        + [dma((tp,))] * 2
        + [dma((ep,))] * 2
        + [dma((4,))] * 2
        + zz * 2,
        compiler_params=pltpu.CompilerParams(
            collective_id=0, has_side_effects=True, vmem_limit_bytes=60 * 1024 * 1024
        ),
    )(
        query_vectors,
        key_vectors,
        value_vectors,
        cos,
        sin,
        query_gain[None, :],
        key_gain[None, :],
        sinks,
        moe_rows,
        norm_gain[None, :],
        table,
        expert_gate,
        expert_up,
        expert_down,
        shared_gate,
        shared_up,
        shared_down,
    )


def choose(*args):
    ep, tp = lax.axis_size("ep"), lax.axis_size("tp")
    query, rows = args[0], args[6]
    kv_heads = args[1].shape[1] // HEAD_DIM
    tok, width = rows.shape
    cap = max(2, 3 * tok * TOP_K // (2 * ep))
    gathered = ep * tok * tp * width * 2
    chunks = query.shape[0] // WINDOW * kv_heads
    fits = (
        gathered <= 16 * 1024 * 1024
        and tp == 4
        and ep % 2 == 0
        and tok % 32 == 0
        and (2 * cap) % 16 == 0
        and cap % 8 == 0
        and chunks % (ep // 2) == 0
    )
    return fast_shards(*args) if fits else shards(*args)


def solution(mesh):
    placed = (
        P("ep", "tp"),
        P("ep", "tp"),
        P("ep", "tp"),
        P(),
        P(),
        P("tp"),
        P("ep", "tp"),
        P(),
        P("ep", None),
        P("ep", None),
        P("ep", None, "tp"),
        P("ep", None, "tp"),
        P("ep", None, "tp"),
        P(None, "tp"),
        P(None, "tp"),
        P(None, "tp"),
    )
    return jax.shard_map(
        choose,
        mesh=mesh,
        in_specs=placed,
        out_specs=(P("ep", "tp"), P("ep", "tp")),
        check_vma=False,
    )
```

```python
import functools

import jax
import jax.numpy as jnp
from jax import lax
from jax.experimental import pallas as pl
from jax.experimental.pallas import tpu as pltpu
from jax.sharding import PartitionSpec as P

HEAD_DIM = 128
WINDOW = 128
GRID_W = 64
D = 4096
TOP_K = 4


epsilon = 1e-06
rotary_base = 10000.0


def padded_2(block, sides, width):
    for axis, dim in sides:
        count = lax.axis_size(axis)
        forward = [(i, i + 1) for i in range(count - 1)]
        backward = [(target, source) for source, target in forward]
        low = lax.ppermute(
            lax.slice_in_dim(block, block.shape[dim] - width, None, axis=dim), axis, forward
        )
        high = lax.ppermute(lax.slice_in_dim(block, 0, width, axis=dim), axis, backward)
        block = jnp.concatenate([low, block, high], axis=dim)
    return block


def half_turn(halves):
    leading, trailing = jnp.split(halves, 2, axis=-1)
    return jnp.concatenate([-trailing, leading], axis=-1)


def rotate_heads(vectors, head_gain, positions):
    floats = vectors.astype(jnp.float32)
    normed = (
        floats * lax.rsqrt(jnp.mean(floats * floats, axis=-1, keepdims=True) + epsilon) * head_gain
    )
    quarter = HEAD_DIM // 4
    freq_index = jnp.arange(quarter, dtype=jnp.int32).astype(jnp.float32)
    inverse = rotary_base ** (-4.0 * freq_index / HEAD_DIM)
    grid_row = (positions // GRID_W).astype(jnp.float32)[:, None] * inverse
    grid_col = (positions % GRID_W).astype(jnp.float32)[:, None] * inverse
    angles = jnp.concatenate([grid_row, grid_row, grid_col, grid_col], axis=-1)[:, None, :]
    row_half, col_half = jnp.split(normed, 2, axis=-1)
    turned = jnp.concatenate([half_turn(row_half), half_turn(col_half)], axis=-1)
    return (normed * jnp.cos(angles) + turned * jnp.sin(angles)).astype(jnp.bfloat16)


def attend_window(query_vectors, key_vectors, value_vectors, query_gain, key_gain, sink_logits):
    length = query_vectors.shape[0]
    heads_here = sink_logits.shape[0]
    kv_here = key_vectors.shape[1] // HEAD_DIM
    grouping = heads_here // kv_here
    shard_start = lax.axis_index("ep") * length
    positions = shard_start + jnp.arange(length, dtype=jnp.int32)
    queries = rotate_heads(
        query_vectors.reshape(length, heads_here, HEAD_DIM), query_gain, positions
    )
    turned_keys = rotate_heads(key_vectors.reshape(length, kv_here, HEAD_DIM), key_gain, positions)
    turned_keys = turned_keys.reshape(length, kv_here * HEAD_DIM)
    padded = padded_2(jnp.stack([turned_keys, value_vectors]), (("ep", 1),), WINDOW)
    extent = length + 2 * WINDOW
    near_keys = padded[0].reshape(extent, kv_here, HEAD_DIM)
    near_values = padded[1].reshape(extent, kv_here, HEAD_DIM)
    key_pos = shard_start - WINDOW + jnp.arange(extent, dtype=jnp.int32)
    inside = (
        (jnp.abs(positions[:, None] - key_pos[None, :]) <= WINDOW)
        & (key_pos >= 0)[None, :]
        & (key_pos < lax.axis_size("ep") * length)[None, :]
    )
    scores = jnp.einsum(
        "qhgd,khd->hgqk",
        queries.reshape(length, kv_here, grouping, HEAD_DIM),
        near_keys,
        preferred_element_type=jnp.float32,
    ) * HEAD_DIM ** (-0.5)
    raised = jnp.where(inside, jnp.exp(scores), 0.0)
    denominator = jnp.exp(sink_logits).reshape(kv_here, grouping)[:, :, None] + jnp.sum(
        raised, axis=-1
    )
    weights = (raised / denominator[..., None]).astype(jnp.bfloat16)
    mixed = jnp.einsum("hgqk,khd->qhgd", weights, near_values, preferred_element_type=jnp.float32)
    return mixed.astype(jnp.bfloat16).reshape(length, heads_here * HEAD_DIM)


def project(block_rows, gain_piece, gate_rows, up_rows):
    floats = block_rows.astype(jnp.float32)
    weighted = (floats * gain_piece).astype(jnp.bfloat16)
    gate_sum = jnp.dot(weighted, gate_rows, preferred_element_type=jnp.float32)
    up_sum = jnp.dot(weighted, up_rows, preferred_element_type=jnp.float32)
    return (gate_sum, up_sum, jnp.sum(floats * floats, axis=1))


def activate(gate_sum, up_sum, squares):
    factor = lax.rsqrt(squares / D + epsilon)[:, None]
    return (jax.nn.silu(gate_sum * factor) * (up_sum * factor)).astype(jnp.bfloat16)


def shards(
    query_vectors,
    key_vectors,
    value_vectors,
    query_gain,
    key_gain,
    sink_logits,
    moe_rows,
    norm_gain,
    expert_ids,
    route_weights,
    expert_gate,
    expert_up,
    expert_down,
    shared_gate,
    shared_up,
    shared_down,
):
    attended = attend_window(
        query_vectors, key_vectors, value_vectors, query_gain, key_gain, sink_logits
    )
    ep_size = lax.axis_size("ep")
    tokens_here, width_here = moe_rows.shape
    capacity = max(2, 3 * tokens_here * TOP_K // (2 * ep_size))
    slots_all = ep_size * capacity
    flat_ids = expert_ids.reshape(-1)
    onehot = (flat_ids[:, None] == jnp.arange(ep_size, dtype=jnp.int32)[None, :]).astype(jnp.int32)
    slot_index = jnp.sum((jnp.cumsum(onehot, axis=0) - onehot) * onehot, axis=1)
    target = flat_ids * capacity + slot_index
    matches = target[None, :] == jnp.arange(slots_all, dtype=jnp.int32)[:, None]
    present = jnp.any(matches, axis=1)
    owner_row = jnp.arange(tokens_here * TOP_K, dtype=jnp.int32) // TOP_K
    source_row = jnp.sum(jnp.where(matches, owner_row[None, :], 0), axis=1)
    local_gate = expert_gate[0]
    local_up = expert_up[0]
    local_down = expert_down[0]
    units_here = local_gate.shape[1]
    shared_units = shared_gate.shape[1]
    outgoing = jnp.where(
        present[:, None], jnp.take(moe_rows, source_row, axis=0), jnp.zeros((), jnp.bfloat16)
    )
    arrived = lax.all_to_all(
        outgoing.reshape(ep_size, capacity, width_here),
        "ep",
        split_axis=0,
        concat_axis=0,
        tiled=True,
    )
    arrived = arrived.reshape(slots_all, width_here)
    routed = project(
        lax.all_gather(arrived, "tp", axis=1, tiled=True), norm_gain, local_gate, local_up
    )
    shared = project(
        lax.all_gather(moe_rows, "tp", axis=1, tiled=True), norm_gain, shared_gate, shared_up
    )
    gate_sum, up_sum, squares, shared_gsum, shared_usum, own_squares = tuple(
        (new_term for new_term in routed + shared)
    )
    hidden = activate(gate_sum, up_sum, squares)
    shared_hidden = activate(shared_gsum, shared_usum, own_squares)
    packing = units_here // shared_units
    stacked = jnp.concatenate(
        [hidden, shared_hidden.reshape(tokens_here // packing, units_here)], axis=0
    )
    columns = local_down.shape[1]
    portion = lax.all_gather(stacked, "tp", axis=1, tiled=True)
    shards_in = portion.shape[1] // units_here
    routed = jnp.dot(portion[:slots_all], local_down, preferred_element_type=jnp.float32)
    shared_piece = portion[slots_all:].reshape(
        tokens_here // packing, shards_in, packing, shared_units
    )
    shared_piece = shared_piece.transpose(0, 2, 1, 3).reshape(tokens_here, shards_in * shared_units)
    shared = jnp.dot(shared_piece, shared_down, preferred_element_type=jnp.float32)
    returned = lax.all_to_all(
        routed.astype(jnp.bfloat16).reshape(ep_size, capacity, columns),
        "ep",
        split_axis=0,
        concat_axis=0,
        tiled=True,
    )
    returned = returned.reshape(slots_all, columns)
    picked = jnp.take(returned, target, axis=0).reshape(tokens_here, TOP_K, columns)
    combined = shared + jnp.sum(route_weights[:, :, None] * picked.astype(jnp.float32), axis=1)
    return (attended, combined.astype(jnp.bfloat16))


F32 = jnp.float32
BF16 = jnp.bfloat16
MESH = pl.DeviceIdType.MESH
LANES = 128


def moe_kernel(
    sizes,
    q_hbm,
    k_hbm,
    v_hbm,
    cos_ref,
    sin_ref,
    qgain_ref,
    kgain_ref,
    sink_ref,
    x_hbm,
    gain_ref,
    wt_hbm,
    gate_hbm,
    up_hbm,
    down_hbm,
    sgate_hbm,
    sup_hbm,
    sdown_hbm,
    att_ref,
    out_ref,
    xbuf,
    gate,
    up,
    down,
    sgate,
    sup,
    sdown,
    qbuf,
    kbuf,
    vbuf,
    wbuf,
    scaled,
    factor,
    hid,
    hbuf,
    shbuf,
    pbuf,
    prx,
    qtx,
    qrx,
    local_sem,
    zs,
    zr,
    xs,
    xr,
    ys,
    yr,
    dxs,
    dxr,
    dys,
    dyr,
    ps,
    pr,
    hxs,
    hxr,
    hys,
    hyr,
    gxs,
    gxr,
    gys,
    gyr,
    ss,
    sr,
    ws,
    wr,
    ks,
    kr,
    pps,
    ppr,
    qqs,
    qqr,
):
    ep, tp, nz, tok, width, cap, tok_a, kv_heads, group, units, columns, sunits = sizes
    e = lax.axis_index("ep")
    t = lax.axis_index("tp")
    z, c = e // 2, e % 2
    other = 1 - c
    partner = z * 2 + other
    tx, ty = t % 2, t // 2
    xn = ty * 2 + (1 - tx)
    yn = (1 - ty) * 2 + tx
    dn = (1 - ty) * 2 + (1 - tx)
    half = tok // 2
    slots = 2 * cap
    hcut = (slots // 2 + 15) // 16 * 16
    row_c = pl.multiple_of(c * tok, 16)
    row_o = pl.multiple_of(other * tok, 16)

    def rc(src, dst, s_sem, r_sem, dev):
        return pltpu.make_async_remote_copy(
            src_ref=src,
            dst_ref=dst,
            send_sem=s_sem,
            recv_sem=r_sem,
            device_id=dev,
            device_id_type=MESH,
        )

    unit0 = xbuf.at[z, t, pl.ds(row_c, tok), :]
    loads = [
        (x_hbm, unit0),
        (wt_hbm, wbuf.at[e]),
        (k_hbm, kbuf.at[pl.ds(WINDOW, tok_a), :]),
        (v_hbm, vbuf.at[pl.ds(WINDOW, tok_a), :]),
        (q_hbm, qbuf),
        (gate_hbm.at[0], gate),
        (up_hbm.at[0], up),
        (sgate_hbm, sgate),
        (sup_hbm, sup),
        (down_hbm.at[0], down),
        (sdown_hbm, sdown),
    ]
    copies = [
        pltpu.make_async_copy(a, b, local_sem.at[i]) for i, (a, b) in enumerate(loads)
    ]
    for cp in copies:
        cp.start()

    barrier = pltpu.get_barrier_semaphore()
    for d in range(1, ep):
        pl.semaphore_signal(barrier, inc=1, device_id=((e + d) % ep, t), device_id_type=MESH)
    for d in range(1, tp):
        pl.semaphore_signal(barrier, inc=1, device_id=(e, (t + d) % tp), device_id_type=MESH)
    pl.semaphore_wait(barrier, ep + tp - 2)

    def unit(zi, ti, row, first=0, count=tok):
        return xbuf.at[zi, ti, pl.ds(row + first, count), :]

    def z_copy(d):
        zi = (z + d) % nz
        return rc(unit0, unit0, zs.at[d], zr.at[z], (zi * 2 + c, t))

    def z_landed(zi):
        u = unit(zi, t, row_c)
        return rc(u, u, zs.at[0], zr.at[zi], (e, xn))

    def x_copy(zi):
        u = unit(zi, t, row_c)
        return rc(u, u, xs.at[zi], xr.at[zi], (e, xn))

    def y_copy(zi):
        u = unit(zi, t, row_c)
        return rc(u, u, ys.at[zi], yr.at[zi], (e, yn))

    def x_landed(zi):
        u = unit(zi, xn, row_c)
        return rc(u, u, xs.at[zi], xr.at[zi], (e, xn))

    def y_landed(zi):
        u = unit(zi, yn, row_c)
        return rc(u, u, ys.at[zi], yr.at[zi], (e, yn))

    def dy_copy(zi):
        u = unit(zi, xn, row_c, 0, half)
        return rc(u, u, dys.at[zi], dyr.at[zi], (e, yn))

    def dx_copy(zi):
        u = unit(zi, yn, row_c, half, half)
        return rc(u, u, dxs.at[zi], dxr.at[zi], (e, xn))

    def dy_landed(zi):
        u = unit(zi, dn, row_c, 0, half)
        return rc(u, u, dys.at[zi], dyr.at[zi], (e, yn))

    def dx_landed(zi):
        u = unit(zi, dn, row_c, half, half)
        return rc(u, u, dxs.at[zi], dxr.at[zi], (e, xn))

    def p_copy(zi, ti):
        u = unit(zi, ti, row_c)
        return rc(u, u, ps.at[zi, ti], pr.at[zi, ti], (partner, t))

    def p_landed(zi, ti):
        u = unit(zi, ti, row_o)
        return rc(u, u, ps.at[zi, ti], pr.at[zi, ti], (partner, t))

    def hx_copy(zi):
        u = hbuf.at[zi, t]
        return rc(u, u, hxs.at[zi], hxr.at[zi], (e, xn))

    def hy_copy(zi):
        u = hbuf.at[zi, t]
        return rc(u, u, hys.at[zi], hyr.at[zi], (e, yn))

    def hx_landed(zi):
        u = hbuf.at[zi, xn]
        return rc(u, u, hxs.at[zi], hxr.at[zi], (e, xn))

    def hy_landed(zi):
        u = hbuf.at[zi, yn]
        return rc(u, u, hys.at[zi], hyr.at[zi], (e, yn))

    def gy_copy(zi):
        u = hbuf.at[zi, xn, pl.ds(0, hcut), :]
        return rc(u, u, gys.at[zi], gyr.at[zi], (e, yn))

    def gx_copy(zi):
        u = hbuf.at[zi, yn, pl.ds(hcut, slots - hcut), :]
        return rc(u, u, gxs.at[zi], gxr.at[zi], (e, xn))

    def gy_landed(zi):
        u = hbuf.at[zi, dn, pl.ds(0, hcut), :]
        return rc(u, u, gys.at[zi], gyr.at[zi], (e, yn))

    def gx_landed(zi):
        u = hbuf.at[zi, dn, pl.ds(hcut, slots - hcut), :]
        return rc(u, u, gxs.at[zi], gxr.at[zi], (e, xn))

    def s_copy(d):
        u = shbuf.at[t]
        return rc(u, u, ss.at[d], sr.at[t], (e, (t + d) % tp))

    def s_landed(ti):
        u = shbuf.at[ti]
        return rc(u, u, ss.at[0], sr.at[ti], (e, xn))

    def w_copy(d):
        u = wbuf.at[e]
        return rc(u, u, ws.at[d], wr.at[e], ((e + d) % ep, t))

    def w_landed(ei):
        u = wbuf.at[ei]
        return rc(u, u, ws.at[0], wr.at[ei], (partner, t))

    after, before = (e + 1) % ep, (e + ep - 1) % ep
    tail = pl.ds(tok_a, WINDOW)
    first = pl.ds(WINDOW, WINDOW)
    low = pl.ds(0, WINDOW)
    high = pl.ds(WINDOW + tok_a, WINDOW)
    halos = [
        rc(kbuf.at[tail, :], kbuf.at[low, :], ks.at[0], kr.at[0], (after, t)),
        rc(kbuf.at[first, :], kbuf.at[high, :], ks.at[1], kr.at[1], (before, t)),
        rc(vbuf.at[tail, :], vbuf.at[low, :], ks.at[2], kr.at[2], (after, t)),
        rc(vbuf.at[first, :], vbuf.at[high, :], ks.at[3], kr.at[3], (before, t)),
    ]

    def pp_copy(zi):
        return rc(pbuf.at[zi, other], prx.at[zi], pps.at[zi], ppr.at[zi], (partner, t))

    def qq_copy(zi):
        return rc(qtx.at[zi], qrx.at[z], qqs.at[zi], qqr.at[z], (zi * 2 + c, t))

    def qq_landed(zi):
        return rc(qrx.at[zi], qrx.at[zi], qqs.at[zi], qqr.at[zi], (partner, t))

    copies[0].wait()
    x_copy(z).start()
    y_copy(z).start()
    for d in range(1, nz):
        z_copy(d).start()
    p_copy(z, t).start()
    copies[1].wait()
    for d in range(1, ep):
        w_copy(d).start()
    copies[2].wait()
    copies[3].wait()
    for h in halos:
        h.start()
    copies[4].wait()

    lane = lax.broadcasted_iota(jnp.int32, (WINDOW, LANES), 1)
    leading = (lane % (HEAD_DIM // 2)) < HEAD_DIM // 4

    def turn(block, head_gain, table_rows):
        v = block.astype(F32)
        v = v * lax.rsqrt(jnp.mean(v * v, axis=-1, keepdims=True) + epsilon) * head_gain
        swapped = jnp.where(
            leading,
            pltpu.roll(v, HEAD_DIM - HEAD_DIM // 4, 1),
            pltpu.roll(v, HEAD_DIM // 4, 1),
        )
        return (v * cos_ref[table_rows, :] + swapped * sin_ref[table_rows, :]).astype(BF16)

    heads = kv_heads * group

    def turn_q(i, carry):
        rows = pl.ds(pl.multiple_of(i * WINDOW, WINDOW), WINDOW)
        table = pl.ds(pl.multiple_of((i + 1) * WINDOW, WINDOW), WINDOW)
        for h in range(heads):
            cols = slice(h * HEAD_DIM, (h + 1) * HEAD_DIM)
            qbuf[rows, cols] = turn(qbuf[rows, cols], qgain_ref[...], table)
        return carry

    nq = tok_a // WINDOW
    lax.fori_loop(0, nq, turn_q, 0)

    def forward_z(zi):
        z_landed(zi).wait_recv()
        x_copy(zi).start()
        y_copy(zi).start()
        p_copy(zi, t).start()

    forward_z((z + 1) % nz)

    for h in halos:
        h.wait()

    def turn_k(i, carry):
        rows = pl.ds(pl.multiple_of(i * WINDOW, WINDOW), WINDOW)
        for h in range(kv_heads):
            cols = slice(h * HEAD_DIM, (h + 1) * HEAD_DIM)
            kbuf[rows, cols] = turn(kbuf[rows, cols], kgain_ref[...], rows)
        return carry

    lax.fori_loop(0, nq + 2, turn_k, 0)
    for d in range(1, ep):
        w_landed((e + d) % ep).wait_recv()
    for cp in copies[5:]:
        cp.wait()

    span = 3 * WINDOW

    def attend(i, carry):
        qb, kh = i // kv_heads, i % kv_heads
        rows = pl.ds(pl.multiple_of(qb * WINDOW, WINDOW), WINDOW)
        keys = pl.ds(pl.multiple_of(qb * WINDOW, WINDOW), span)
        kcols = pl.ds(pl.multiple_of(kh * HEAD_DIM, HEAD_DIM), HEAD_DIM)
        near = lax.broadcasted_iota(jnp.int32, (WINDOW, span), 1)
        mine = lax.broadcasted_iota(jnp.int32, (WINDOW, span), 0)
        pos = e * tok_a + (qb - 1) * WINDOW + near
        inside = (
            (near - mine >= 0) & (near - mine <= 2 * WINDOW) & (pos >= 0) & (pos < ep * tok_a)
        )
        kk = kbuf[keys, kcols]
        vv = vbuf[keys, kcols]
        for g in range(group):
            qcols = pl.ds(
                pl.multiple_of((kh * group + g) * HEAD_DIM, HEAD_DIM), HEAD_DIM
            )
            scores = lax.dot_general(
                qbuf[rows, qcols], kk, (((1,), (1,)), ((), ())), preferred_element_type=F32
            )
            raised = jnp.where(inside, jnp.exp(scores * HEAD_DIM ** (-0.5)), 0.0)
            sink = jnp.exp(sink_ref[kh * group + g])
            total = jnp.sum(raised, axis=-1, keepdims=True) + sink[0:1, 0:1]
            weights = (raised * (1.0 / total)).astype(BF16)
            att_ref[rows, qcols] = jnp.dot(weights, vv, preferred_element_type=F32).astype(BF16)
        return carry

    upper = (
        lax.broadcasted_iota(jnp.int32, (tok, tok), 0)
        < lax.broadcasted_iota(jnp.int32, (tok, tok), 1)
    ).astype(F32)

    def picks(block):
        weight = wbuf[block, pl.ds(e, 1), :][:, :tok]
        named = jnp.where(weight > 0.0, 1.0, 0.0)
        rank = jnp.dot(
            jnp.broadcast_to(named, (16, tok)).astype(BF16),
            upper.astype(BF16),
            preferred_element_type=F32,
        )[0:1, :]
        slot = lax.broadcasted_iota(jnp.int32, (cap, tok), 0).astype(F32)
        hot = jnp.where((slot == rank) & (named > 0.0), 1.0, 0.0)
        return hot, jnp.sum(hot * weight, axis=1, keepdims=True)

    chunk = 32

    def silu_pair(g, u, f):
        g = g * f
        return g / (1.0 + jnp.exp(-g)) * (u * f)

    tile = min(256, units)

    def project_pair(zi):
        def scale(i, carry):
            rows = pl.ds(pl.multiple_of(i * chunk, chunk), chunk)
            squares = jnp.zeros((chunk, 1), F32)
            for ti in range(tp):
                v = xbuf[zi, ti, rows, :].astype(F32)
                squares += jnp.sum(v * v, axis=1, keepdims=True)
                cols = slice(ti * width, (ti + 1) * width)
                scaled[rows, cols] = (v * gain_ref[:, cols]).astype(BF16)
            f = lax.rsqrt(squares / (tp * width) + epsilon)
            factor[rows, :] = jnp.broadcast_to(f, (chunk, LANES))
            return carry

        lax.fori_loop(0, 2 * tok // chunk, scale, 0)

        def columns_of(n, carry):
            cols = pl.ds(pl.multiple_of(n * tile, tile), tile)
            g = jnp.dot(scaled[...], gate[:, cols], preferred_element_type=F32)
            u = jnp.dot(scaled[...], up[:, cols], preferred_element_type=F32)
            hid[:, cols] = silu_pair(g, u, factor[:, 0:1]).astype(BF16)
            return carry

        lax.fori_loop(0, units // tile, columns_of, 0)
        parts = []
        for ci in range(2):
            hot, _ = picks(zi * 2 + ci)
            parts.append(
                jnp.dot(
                    hot.astype(BF16),
                    hid[ci * tok : (ci + 1) * tok, :],
                    preferred_element_type=F32,
                )
            )
        hbuf[zi, t] = jnp.concatenate(parts, axis=0).astype(BF16)

    def shared_up():
        rows = pl.ds(row_c, tok)
        g = jnp.dot(scaled[rows, :], sgate[...], preferred_element_type=F32)
        u = jnp.dot(scaled[rows, :], sup[...], preferred_element_type=F32)
        shbuf[t] = silu_pair(g, u, factor[rows, 0:1]).astype(BF16)

    ctile = min(256, columns)

    def down_pair(zi):
        picked = [picks(zi * 2 + ci) for ci in range(2)]
        slot_weight = jnp.concatenate([p[1] for p in picked], axis=0)

        def columns_of(n, carry):
            cols = pl.ds(pl.multiple_of(n * ctile, ctile), ctile)
            acc = jnp.zeros((slots, ctile), F32)
            for ti in range(tp):
                acc += jnp.dot(
                    hbuf[zi, ti],
                    down[ti * units : (ti + 1) * units, cols],
                    preferred_element_type=F32,
                )
            weighted = acc.astype(BF16).astype(F32) * slot_weight
            for ci in range(2):
                spread = lax.dot_general(
                    picked[ci][0].astype(BF16),
                    weighted[ci * cap : (ci + 1) * cap, :].astype(BF16),
                    (((0,), (0,)), ((), ())),
                    preferred_element_type=F32,
                )
                pbuf[zi, ci, :, cols] = spread.astype(BF16)
            return carry

        lax.fori_loop(0, columns // ctile, columns_of, 0)

    per_step = nq * kv_heads // nz

    def step(s, carry):
        @pl.when(s < nz)
        def _():
            lax.fori_loop(s * per_step, (s + 1) * per_step, attend, 0)
            zi = (z + s) % nz
            x_landed(zi).wait_recv()
            dy_copy(zi).start()
            p_copy(zi, xn).start()
            y_landed(zi).wait_recv()
            dx_copy(zi).start()
            p_copy(zi, yn).start()

            @pl.when(s + 2 < nz)
            def _():
                forward_z((z + s + 2) % nz)

            dy_landed(zi).wait_recv()
            dx_landed(zi).wait_recv()
            p_copy(zi, dn).start()
            for ti in range(tp):
                p_landed(zi, ti).wait_recv()
            project_pair(zi)
            hx_copy(zi).start()
            hy_copy(zi).start()

            @pl.when(s == 0)
            def _():
                shared_up()
                for d in range(1, tp):
                    s_copy(d).start()

        @pl.when((s >= 1) & (s < nz + 1))
        def _():
            zi = (z + s - 1) % nz
            hx_landed(zi).wait_recv()
            gy_copy(zi).start()
            hy_landed(zi).wait_recv()
            gx_copy(zi).start()

        @pl.when((s >= 2) & (s < nz + 2))
        def _():
            zi = (z + s - 2) % nz
            gy_landed(zi).wait_recv()
            gx_landed(zi).wait_recv()
            down_pair(zi)
            pp_copy(zi).start()
            pp_copy(zi).wait_recv()
            qtx[zi] = (pbuf[zi, c].astype(F32) + prx[zi].astype(F32)).astype(BF16)

            @pl.when(s > 2)
            def _():
                qq_copy(zi).start()

        return carry

    lax.fori_loop(0, nz + 2, step, 0)

    for d in range(1, tp):
        s_landed((t + d) % tp).wait_recv()
    for d in range(1, nz):
        qq_landed((z + d) % nz).wait_recv()
    for n in range(columns // ctile):
        cols = slice(n * ctile, (n + 1) * ctile)
        acc = qtx[z, :, cols].astype(F32)
        for d in range(1, nz):
            acc += qrx[(z + d) % nz, :, cols].astype(F32)
        for ti in range(tp):
            acc += jnp.dot(
                shbuf[ti],
                sdown[ti * sunits : (ti + 1) * sunits, cols],
                preferred_element_type=F32,
            )
        out_ref[:, cols] = acc.astype(BF16)

    for d in range(1, nz):
        z_copy(d).wait_send()
        qq_copy((z + d) % nz).wait_send()
    for d in range(1, tp):
        s_copy(d).wait_send()
    for d in range(1, ep):
        w_copy(d).wait_send()

    def drain(zi, carry):
        for kind in (x_copy, y_copy, dx_copy, dy_copy, hx_copy, hy_copy, gx_copy, gy_copy, pp_copy):
            kind(zi).wait_send()
        for ti in range(tp):
            p_copy(zi, ti).wait_send()
        return carry

    lax.fori_loop(0, nz, drain, 0)


def fast_shards(
    query_vectors,
    key_vectors,
    value_vectors,
    query_gain,
    key_gain,
    sink_logits,
    moe_rows,
    norm_gain,
    expert_ids,
    route_weights,
    expert_gate,
    expert_up,
    expert_down,
    shared_gate,
    shared_up,
    shared_down,
):
    ep, tp = lax.axis_size("ep"), lax.axis_size("tp")
    nz = ep // 2
    tok, width = moe_rows.shape
    cap = max(2, 3 * tok * TOP_K // (2 * ep))
    tok_a = query_vectors.shape[0]
    heads = sink_logits.shape[0]
    kv_heads = key_vectors.shape[1] // HEAD_DIM
    group = heads // kv_heads
    units = expert_gate.shape[2]
    columns = expert_down.shape[2]
    sunits = shared_gate.shape[1]
    sizes = (ep, tp, nz, tok, width, cap, tok_a, kv_heads, group, units, columns, sunits)
    full = tp * width

    extent = tok_a + 2 * WINDOW
    first_row = (lax.axis_index("ep") * tok_a - WINDOW) // GRID_W
    grid_rows = extent // GRID_W
    quarter = HEAD_DIM // 4
    inverse = rotary_base ** (-4.0 * jnp.arange(quarter, dtype=jnp.int32).astype(F32) / HEAD_DIM)
    row_ids = first_row + jnp.arange(grid_rows, dtype=jnp.int32)
    grid_row = row_ids.astype(F32)[:, None] * inverse
    grid_col = jnp.arange(GRID_W, dtype=jnp.int32).astype(F32)[:, None] * inverse

    def by_row(a):
        return jnp.broadcast_to(a[:, None, :], (grid_rows, GRID_W, quarter)).reshape(extent, quarter)

    def by_col(a):
        return jnp.broadcast_to(a[None], (grid_rows, GRID_W, quarter)).reshape(extent, quarter)

    cr, sr = by_row(jnp.cos(grid_row)), by_row(jnp.sin(grid_row))
    cc, sc = by_col(jnp.cos(grid_col)), by_col(jnp.sin(grid_col))
    cos = jnp.concatenate([cr, cr, cc, cc], axis=-1)
    sin = jnp.concatenate([-sr, sr, -sc, sc], axis=-1)

    experts = jnp.arange(ep, dtype=jnp.int32)
    table = jnp.sum(
        jnp.where(expert_ids.T[None, :, :] == experts[:, None, None], route_weights.T[None], 0.0),
        axis=1,
    )
    padded_tok = (tok + LANES - 1) // LANES * LANES
    table = jnp.pad(table, ((0, 0), (0, padded_tok - tok)))
    sinks = jnp.broadcast_to(sink_logits[:, None, None], (heads, 8, LANES))

    vm = pl.BlockSpec(memory_space=pltpu.VMEM)
    hb = pl.BlockSpec(memory_space=pl.ANY)
    dma = pltpu.SemaphoreType.DMA
    slots = 2 * cap
    zz = [dma((nz,))] * 2
    return pl.pallas_call(
        functools.partial(moe_kernel, sizes),
        out_shape=(
            jax.ShapeDtypeStruct((tok_a, heads * HEAD_DIM), BF16),
            jax.ShapeDtypeStruct((tok, columns), BF16),
        ),
        in_specs=[hb, hb, hb, vm, vm, vm, vm, vm, hb, vm, hb, hb, hb, hb, hb, hb, hb],
        out_specs=(vm, vm),
        scratch_shapes=[
            pltpu.VMEM((nz, tp, 2 * tok, width), BF16),
            pltpu.VMEM((full, units), BF16),
            pltpu.VMEM((full, units), BF16),
            pltpu.VMEM((tp * units, columns), BF16),
            pltpu.VMEM((full, sunits), BF16),
            pltpu.VMEM((full, sunits), BF16),
            pltpu.VMEM((tp * sunits, columns), BF16),
            pltpu.VMEM((tok_a, heads * HEAD_DIM), BF16),
            pltpu.VMEM((extent, kv_heads * HEAD_DIM), BF16),
            pltpu.VMEM((extent, kv_heads * HEAD_DIM), BF16),
            pltpu.VMEM((ep, ep, padded_tok), F32),
            pltpu.VMEM((2 * tok, full), BF16),
            pltpu.VMEM((2 * tok, LANES), F32),
            pltpu.VMEM((2 * tok, units), BF16),
            pltpu.VMEM((nz, tp, slots, units), BF16),
            pltpu.VMEM((tp, tok, sunits), BF16),
            pltpu.VMEM((nz, 2, tok, columns), BF16),
            pltpu.VMEM((nz, tok, columns), BF16),
            pltpu.VMEM((nz, tok, columns), BF16),
            pltpu.VMEM((nz, tok, columns), BF16),
            dma((11,)),
        ]
        + zz * 5
        + [dma((nz, tp))] * 2
        + zz * 4
        + [dma((tp,))] * 2
        + [dma((ep,))] * 2
        + [dma((4,))] * 2
        + zz * 2,
        compiler_params=pltpu.CompilerParams(
            collective_id=0, has_side_effects=True, vmem_limit_bytes=60 * 1024 * 1024
        ),
    )(
        query_vectors,
        key_vectors,
        value_vectors,
        cos,
        sin,
        query_gain[None, :],
        key_gain[None, :],
        sinks,
        moe_rows,
        norm_gain[None, :],
        table,
        expert_gate,
        expert_up,
        expert_down,
        shared_gate,
        shared_up,
        shared_down,
    )


def choose(*args):
    ep, tp = lax.axis_size("ep"), lax.axis_size("tp")
    query, rows = args[0], args[6]
    kv_heads = args[1].shape[1] // HEAD_DIM
    tok, width = rows.shape
    cap = max(2, 3 * tok * TOP_K // (2 * ep))
    gathered = ep * tok * tp * width * 2
    chunks = query.shape[0] // WINDOW * kv_heads
    fits = (
        gathered <= 16 * 1024 * 1024
        and tp == 4
        and ep % 2 == 0
        and tok % 32 == 0
        and (2 * cap) % 16 == 0
        and cap % 8 == 0
        and query.shape[0] % GRID_W == 0
        and chunks % (ep // 2) == 0
    )
    return fast_shards(*args) if fits else shards(*args)


def solution(mesh):
    placed = (
        P("ep", "tp"),
        P("ep", "tp"),
        P("ep", "tp"),
        P(),
        P(),
        P("tp"),
        P("ep", "tp"),
        P(),
        P("ep", None),
        P("ep", None),
        P("ep", None, "tp"),
        P("ep", None, "tp"),
        P("ep", None, "tp"),
        P(None, "tp"),
        P(None, "tp"),
        P(None, "tp"),
    )
    return jax.shard_map(
        choose,
        mesh=mesh,
        in_specs=placed,
        out_specs=(P("ep", "tp"), P("ep", "tp")),
        check_vma=False,
    )
```
